512 devices in a mesh: fs: 64 (over z, y), tp: 8 (over x, core).
Axes of the slice: x: 4, y: 4, z: 16, core: 2. Of those that a mesh axis runs over, the one named last changes fastest.
Arguments:
- fwd_input: bfloat16 [8192, 2048], P('fs'), may hold values from -6 to 6
- saved_input: bfloat16 [8192, 2048], P('fs'), may hold values from -16 to 16
- out_cotangent: bfloat16 [8192, 2048], P('fs'), may hold values from -16 to 16
- up_weight: bfloat16 [2048, 4096], P('fs', 'tp'), may hold values from -0.125 to 0.125
- down_weight: bfloat16 [4096, 2048], P('tp', 'fs'), may hold values from -0.09375 to 0.09375
- up_grad_sum: float32 [2048, 4096], P('fs', 'tp'), may hold values from -6 to 6
Outputs:
- layer_out: bfloat16 [8192, 2048], P('fs')
- input_grad: bfloat16 [8192, 2048], P('fs')
- up_grad_out: float32 [2048, 4096], P('fs', 'tp')
The draws below stay inside these ranges and needn't reach their ends.
All inputs are finite; a program needn't handle non-finite values.
Results may differ from the reference program's by a relative error of at most 0.013.
Values may be sent and summed in bfloat16 or wider, within the bound.
A program may use at most 64 MiB of HBM per device.

```python
import jax
import jax.numpy as jnp
from jax import lax

D = 2048
FF = 4096
TOKENS = 8192
N_TP = 8


def spiked(entries, key, source, target, parts, factor):
    owner, partner = [(jnp.arange(entries.shape[axis_at]) // (entries.shape[axis_at] // parts)).reshape([-1 if axis == axis_at else 1 for axis in range(entries.ndim)]) for axis_at in (source, target)]
    chosen = jax.random.permutation(key, parts)[partner]
    strong = (owner == chosen) | (owner == (partner + parts // 2) % parts)
    return jnp.where(strong, factor * entries, entries)


def level_of(own_key, dims, cuts, least, top_value):
    loudness, own = 1.0, jax.random.fold_in(own_key, 6)
    for position, shards_of in cuts:
        steps = jnp.exp(jax.random.uniform(jax.random.fold_in(own, position), (shards_of,), jnp.float32, least / len(cuts), top_value / len(cuts)))
        loudness = loudness * jnp.repeat(steps, dims[position] // shards_of).reshape([-1 if axis == position else 1 for axis in range(len(dims))])
    return loudness


def centred(stream_key, dims, spread, limit, cuts=(), held_as=jnp.bfloat16):
    loudness = level_of(stream_key, dims, cuts, -0.22, 0.18) if cuts else 1.0
    drawn = jax.random.normal(stream_key, dims, jnp.float32) * spread * loudness
    return jnp.minimum(jnp.maximum(drawn, -limit), limit).astype(held_as)


def bell_draw_with(key, shape, scale, most, pieces, heavy, dtype=jnp.bfloat16):
    values = scale * jax.random.normal(key, shape, jnp.float32)
    if pieces:
        values = values * level_of(key, shape, pieces, -0.22, 0.18)
    return jnp.clip(spiked(values, jax.random.fold_in(key, 3), *heavy), -most, most).astype(dtype)


def setup_inputs(seed: int = 0) -> dict:
    splits = jax.random.split(jax.random.key(seed), 7)
    fwd_input = centred(splits[0], (TOKENS, D), 1.0, 6.0, ((0, 64),))
    saved_input = bell_draw_with(splits[1], (TOKENS, D), 1.0, 16.0, ((0, 64),), (0, 1, 64, 4.0))
    out_cotangent = bell_draw_with(splits[2], (TOKENS, D), 1.0, 16.0, ((0, 64),), (0, 1, 64, 4.0))
    up_weight = centred(splits[3], (D, FF), D ** -0.5, 0.125, ((0, 64), (1, 8)))
    down_weight = centred(splits[4], (FF, D), FF ** -0.5, 0.09375, ((0, 8), (1, 64)))
    up_grad_sum = centred(splits[5], (D, FF), 1.0, 6.0, ((0, 64), (1, 8)), jnp.float32)
    return {"fwd_input": fwd_input, "saved_input": saved_input, "out_cotangent": out_cotangent, "up_weight": up_weight, "down_weight": down_weight, "up_grad_sum": up_grad_sum}


def split_sum(left, right):
    block = right.shape[0] // N_TP
    running = jnp.zeros((left.shape[0], right.shape[1]), jnp.float32)
    for index in range(N_TP):
        partial_out = jnp.dot(left[:, index * block:(index + 1) * block], right[index * block:(index + 1) * block], preferred_element_type=jnp.float32)
        rounded = lax.optimization_barrier(partial_out.astype(jnp.bfloat16))
        running = running + rounded.astype(jnp.float32)
    return running.astype(jnp.bfloat16)


def reference(fwd_input, saved_input, out_cotangent, up_weight, down_weight, up_grad_sum):
    pre_fwd = jnp.dot(fwd_input, up_weight, preferred_element_type=jnp.float32)
    positive = jnp.maximum(pre_fwd, 0.0)
    hidden = (positive * positive).astype(jnp.bfloat16)
    layer_out = split_sum(hidden, down_weight)
    pre_bwd = jnp.dot(saved_input, up_weight, preferred_element_type=jnp.float32)
    d_hidden = jnp.dot(out_cotangent, down_weight.T, preferred_element_type=jnp.float32)
    d_pre = (d_hidden * 2.0 * jnp.maximum(pre_bwd, 0.0)).astype(jnp.bfloat16)
    input_grad = split_sum(d_pre, up_weight.T)
    up_grad = jnp.dot(saved_input.T, d_pre, preferred_element_type=jnp.float32)
    up_grad_out = up_grad_sum + up_grad * (float(TOKENS) ** -0.5)
    return layer_out, input_grad, up_grad_out
```

```python
import functools

import jax
import jax.numpy as jnp
from jax import lax
from jax.experimental import pallas as pl
from jax.experimental.pallas import tpu as pltpu
from jax.sharding import PartitionSpec as P

MESH = pl.DeviceIdType.MESH
F32 = jnp.float32
BF16 = jnp.bfloat16
B = 4
NX = 4
X_COLS = (256, 384, 256)
O_COLS = (256, 128)


def kernel(
    A, fwd, saved, cot, up, down, out, ing, gout,
    Xb, Wsrc, Wb, H, Pb, Rx0, Rx1, Ry0, Ry1, Sx0, Sx1, Sy0, Sy1, Rz0, Rz1, Rw0, Rw1,
    Gs, Gi, Gc, Gsend, Grecv, Gy,
    lx, lw, wyS, wyR, wS, wR, wcS, wcR, xaS, xaR, xbS, xbR, xcS, xcR,
    gcS, gcR, gS, gR, hS, hR, rxS, rxR, ryS, ryR, rzS, rzR, rwS, rwR, agS, agR, odS, odR,
):
    f, t = lax.axis_index("fs"), lax.axis_index("tp")
    z, p = lax.div(f, B), lax.rem(f, B)
    x, c = lax.div(t, 2), lax.rem(t, 2)
    rows, D = fwd.shape
    half = rows // 2
    Rw, F = up.shape
    Fs = F // B
    quarter = D // NX
    tokens = B * half
    per = A // NX

    peers = [lax.rem(p + i, B) for i in range(1, B)]
    mates = [lax.rem(x + i, NX) for i in range(1, NX)]

    def at_z(d):
        return lax.rem(z + (d + A), A)

    def dev_y(q):
        return (z * B + q, t)

    def dev_x(m):
        return (f, m * 2 + c)

    def dev_z(d):
        return (at_z(d) * B + p, t)

    partner = (f, x * 2 + (1 - c))
    me = (f, t)

    mine = pl.ds(pl.multiple_of(c * Fs, Fs), Fs)
    other = pl.ds(pl.multiple_of((1 - c) * Fs, Fs), Fs)
    my_rows = pl.ds(pl.multiple_of(c * half, half), half)
    its_rows = pl.ds(pl.multiple_of((1 - c) * half, half), half)

    def slice_of(q):
        return pl.ds(pl.multiple_of(q * Fs, Fs), Fs)

    acts = (fwd, saved, cot)
    own = []
    for pc, w in enumerate((up, down)):
        own.append(pltpu.make_async_copy(w, Wsrc.at[pc], lw.at[pc]))
        own.append(
            pltpu.make_async_copy(w.at[:, slice_of(p)], Wb.at[pc, z, p, :, mine], lw.at[2 + pc])
        )
    for j in (1, 2, 0):
        for k in range(NX):
            own.append(
                pltpu.make_async_copy(
                    acts[j].at[my_rows, pl.ds(k * quarter, quarter)], Xb.at[j, p, k], lx.at[j, k]
                )
            )
    for copy in own:
        copy.start()

    barrier = pltpu.get_barrier_semaphore()
    greeted = (
        [dev_y(q) for q in peers] + [dev_x(m) for m in mates] + [partner]
        + [dev_z(d) for d in (1, 2, -1, -2)]
    )
    for device in greeted:
        pl.semaphore_signal(barrier, inc=1, device_id=device, device_id_type=MESH)
    pl.semaphore_wait(barrier, len(greeted))
    for copy in own:
        copy.wait()

    started = []

    def send(src, dst, send_sem, recv_sem, device):
        copy = pltpu.make_async_remote_copy(
            src_ref=src, dst_ref=dst, send_sem=send_sem, recv_sem=recv_sem,
            device_id=device, device_id_type=MESH,
        )
        copy.start()
        started.append(copy)

    def arrived(ref, send_sem, recv_sem, device):
        pltpu.make_async_remote_copy(
            src_ref=ref, dst_ref=ref, send_sem=send_sem, recv_sem=recv_sem,
            device_id=device, device_id_type=MESH,
        ).wait_recv()

    for i, q in enumerate(peers):
        send(
            Wsrc.at[:, :, slice_of(q)], Wb.at[:, z, p, :, mine], wyS.at[i], wyR.at[p], dev_y(q)
        )

    def block(z0, q):
        return Wb.at[:, z0, q, :, mine]

    order = [p] + peers

    def relay(s, d, i):
        way = 1 if s == 0 else -1
        z0, q = at_z(-way * d), order[i]
        for hop in (2, 1):
            if d + hop == A // 2 and (i < B // 2) != (s == 0):
                continue
            send(
                block(z0, q), block(z0, q), wS.at[s, d // 2, i, hop - 1], wR.at[z0, q],
                dev_z(way * hop),
            )

    def w_arrived(z0, q):
        arrived(block(z0, q), wS.at[0, 0, 0, 0], wR.at[z0, q], me)

    for s in range(2):
        relay(s, 0, 0)

    def quarter_part(j, q, m):
        return Xb.at[j, q, m, :, pl.ds(0, X_COLS[j])]

    def rest_part(j, q):
        return Xb.at[j, q, :, :, pl.ds(X_COLS[j], quarter - X_COLS[j])]

    for j in (1, 2, 0):
        for i, q in enumerate(peers):
            send(quarter_part(j, p, x), quarter_part(j, p, x), xaS.at[j, i], xaR.at[j, p], dev_y(q))
    for j in (1, 2, 0):
        for i, q in enumerate(peers):
            send(rest_part(j, p), rest_part(j, p), xbS.at[j, i], xbR.at[j, p], dev_y(q))

    for i, q in enumerate(peers):
        arrived(Wb.at[:, z, q, :, mine], wyS.at[i], wyR.at[q], me)
        for s in range(2):
            relay(s, 0, 1 + i)

    def to_partner(z0):
        there = Wb.at[:, z0, :, :, mine]
        send(there, there, wcS.at[z0], wcR.at[z0], partner)

    to_partner(z)

    def act_share(j):
        for i, q in enumerate(peers):
            arrived(quarter_part(j, q, x), xaS.at[j, i], xaR.at[j, q], me)
            for o, m in enumerate(mates):
                send(
                    quarter_part(j, q, x), quarter_part(j, q, x),
                    xcS.at[j, i, o], xcR.at[j, q, x], dev_x(m),
                )

    def w_round(d):
        for i in range(B):
            for s in range(2):
                way = 1 if s == 0 else -1
                w_arrived(at_z(-way * d), order[i])
                relay(s, d, i)
        for e in (d, d - 1):
            for s in range(2):
                z0 = at_z(-(1 if s == 0 else -1) * e)
                if e != d:
                    for i in range(B):
                        w_arrived(z0, order[i])
                to_partner(z0)

    act_share(1)
    w_round(2)
    act_share(2)
    act_share(0)
    for d in range(4, A // 2, 2):
        w_round(d)
    for e in (A // 2 - 1, 1 - A // 2, A // 2):
        z0 = at_z(e)
        for i in range(B):
            w_arrived(z0, order[i])
        to_partner(z0)

    def act_arrived(j):
        for i, q in enumerate(peers):
            arrived(rest_part(j, q), xbS.at[j, i], xbR.at[j, q], me)
            for o, m in enumerate(mates):
                arrived(quarter_part(j, q, m), xcS.at[j, i, o], xcR.at[j, q, m], me)

    act_arrived(1)
    act_arrived(2)
    for e in range(A):
        there = Wb.at[:, e, :, :, other]
        arrived(there, wcS.at[e], wcR.at[e], me)

    def weights(pc, k):
        return Wb[pc, k * per:(k + 1) * per].reshape(quarter, 2 * Fs)

    def product(j, pc):
        total = jnp.zeros((tokens, 2 * Fs), F32)
        for k in range(NX):
            total += jnp.dot(
                Xb[j, :, k].reshape(tokens, quarter), weights(pc, k), preferred_element_type=F32
            )
        return total

    pre = product(1, 0)
    d_hidden = product(2, 1)
    H[1] = (d_hidden * 2.0 * jnp.maximum(pre, 0.0)).astype(BF16)
    turned = jnp.concatenate([H[1, :, other], H[1, :, mine]], axis=1)
    depth = D // A
    for k in range(NX):
        term = lax.dot_general(
            Xb[1, :, k].reshape(tokens, quarter), turned,
            (((0,), (0,)), ((), ())), preferred_element_type=F32,
        )
        group = pl.ds(k * per, per)
        Gs[group] = term[:, :Fs].astype(BF16).reshape(per, depth, Fs)
        Gc[group] = term[:, Fs:].reshape(per, depth, Fs)
        send(Gs.at[group], Gi.at[group], gcS.at[k], gcR.at[k], partner)

    Rx, Ry, Sx, Sy, Rz, Rq = (Rx0, Rx1), (Ry0, Ry1), (Sx0, Sx1), (Sy0, Sy1), (Rz0, Rz1), (Rw0, Rw1)

    def spread(o, pc):
        for k in range(NX):
            part = lax.dot_general(
                H[o], weights(pc, k), (((1,), (1,)), ((), ())), preferred_element_type=F32
            )
            Pb[o, :, k] = part.astype(BF16).reshape(B, half, quarter)
        v = O_COLS[o]
        for i, m in enumerate(mates):
            send(
                Pb.at[o, :, m, :, pl.ds(0, v)], Rx[o].at[x], rxS.at[o, i], rxR.at[o, x], dev_x(m)
            )
        for i, q in enumerate(peers):
            send(
                Pb.at[o, q, :, :, pl.ds(v, quarter - v)], Ry[o].at[p], ryS.at[o, i], ryR.at[o, p],
                dev_y(q),
            )

    spread(1, 0)

    def g_send(s, d, value):
        way = 1 if s == 0 else -1
        hop = 1 if d % 2 else 2
        Gsend[s, d - 1] = value.astype(BF16)
        send(
            Gsend.at[s, d - 1], Grecv.at[s, d - 1], gS.at[s, d - 1], gR.at[s, d - 1],
            dev_z(way * hop),
        )

    def g_mine(e):
        at = at_z(e)
        return Gc[at] + Gi[at].astype(F32)

    def g_got(s, d):
        arrived(Grecv.at[s, d - 1], gS.at[s, d - 1], gR.at[s, d - 1], me)
        return Grecv[s, d - 1].astype(F32)

    for k in range(NX):
        group = pl.ds(k * per, per)
        arrived(Gi.at[group], gcS.at[k], gcR.at[k], me)
    far = A // 2
    g_send(0, far, g_mine(far))
    for d in range(far - 1, 0, -2):
        for s in range(2):
            g_send(s, d, g_mine(d if s == 0 else -d))

    act_arrived(0)
    positive = jnp.maximum(product(0, 0), 0.0)
    H[0] = (positive * positive).astype(BF16)
    spread(0, 1)

    def g_round(d):
        for s in range(2):
            value = g_mine(d if s == 0 else -d) + g_got(s, d + 1)
            if s == 0 or d + 2 < far:
                value = value + g_got(s, d + 2)
            g_send(s, d, value)

    def x_sums(o):
        v = O_COLS[o]
        for i, m in enumerate(mates):
            arrived(Rx[o].at[m], rxS.at[o, i], rxR.at[o, m], me)
        for i, q in enumerate(peers + [p]):
            total = Pb[o, q, x, :, :v].astype(F32)
            for m in mates:
                total = total + Rx[o][m, q].astype(F32)
            Sx[o][q] = total.astype(BF16)
            if i < len(peers):
                send(Sx[o].at[q], Rz[o].at[p], rzS.at[o, i], rzR.at[o, p], dev_y(q))

    def y_sums(o):
        v = O_COLS[o]
        for i, q in enumerate(peers):
            arrived(Ry[o].at[q], ryS.at[o, i], ryR.at[o, q], me)
        for i, m in enumerate(mates + [x]):
            total = Pb[o, p, m, :, v:].astype(F32)
            for q in peers:
                total = total + Ry[o][q, m].astype(F32)
            Sy[o][m] = total.astype(BF16)
            if i < len(mates):
                send(Sy[o].at[m], Rq[o].at[x], rwS.at[o, i], rwR.at[o, x], dev_x(m))

    outs = (out, ing)

    def piece(o, m, which):
        return outs[o].at[which, pl.ds(pl.multiple_of(m * quarter, quarter), quarter)]

    def finish(o):
        v = O_COLS[o]
        for i, q in enumerate(peers):
            arrived(Rz[o].at[q], rzS.at[o, i], rzR.at[o, q], me)
        total = Sx[o][p].astype(F32)
        for q in peers:
            total = total + Rz[o][q].astype(F32)
        left = total.astype(BF16)
        for i, m in enumerate(mates):
            arrived(Rq[o].at[m], rwS.at[o, i], rwR.at[o, m], me)
        total = Sy[o][x].astype(F32)
        for m in mates:
            total = total + Rq[o][m].astype(F32)
        outs[o][my_rows, pl.ds(pl.multiple_of(x * quarter, quarter), quarter)] = jnp.concatenate(
            [left, total.astype(BF16)], axis=1
        )
        for i, m in enumerate(mates):
            send(piece(o, x, my_rows), piece(o, x, my_rows), agS.at[o, i], agR.at[o, x], dev_x(m))
        send(piece(o, x, my_rows), piece(o, x, my_rows), odS.at[o, x], odR.at[o, x], partner)

    def pass_on(o):
        for i, m in enumerate(mates):
            arrived(piece(o, m, my_rows), agS.at[o, i], agR.at[o, m], me)
            send(piece(o, m, my_rows), piece(o, m, my_rows), odS.at[o, m], odR.at[o, m], partner)

    g_round(6)
    x_sums(1)
    y_sums(1)
    g_round(4)
    x_sums(0)
    y_sums(0)
    g_round(2)
    finish(1)

    total = g_mine(0)
    for s in range(2):
        for d in (1, 2):
            total = total + g_got(s, d)
    Gy[...] = total.astype(BF16).reshape(B, Rw, Fs)
    for i, q in enumerate(peers):
        send(Gy.at[q], gout.at[:, slice_of(p)], hS.at[i], hR.at[p], dev_y(q))
    gout[:, slice_of(p)] = Gy[p]

    finish(0)
    pass_on(1)
    pass_on(0)
    for i, q in enumerate(peers):
        arrived(gout.at[:, slice_of(q)], hS.at[i], hR.at[q], me)
    for o in (1, 0):
        for m in range(NX):
            arrived(piece(o, m, its_rows), odS.at[o, m], odR.at[o, m], me)
    for copy in started:
        copy.wait_send()


def per_device(n, T, fwd_input, saved_input, out_cotangent, up_weight, down_weight, up_grad_sum):
    rows, D = fwd_input.shape
    Rw, F = up_weight.shape
    A = n // B
    Fs, half, quarter, depth = F // B, rows // 2, D // NX, D // A
    dma = pltpu.SemaphoreType.DMA
    flops = 12 * B * half * 2 * Fs * D
    anywhere = pl.BlockSpec(memory_space=pl.ANY)
    vmem = pl.BlockSpec(memory_space=pltpu.VMEM)
    v = O_COLS
    u = tuple(quarter - w for w in v)

    def pair(*shapes):
        return [pltpu.VMEM(shape, BF16) for shape in shapes]

    layer_out, input_grad, grad = pl.pallas_call(
        functools.partial(kernel, A),
        out_shape=(
            jax.ShapeDtypeStruct((rows, D), BF16),
            jax.ShapeDtypeStruct((rows, D), BF16),
            jax.ShapeDtypeStruct((Rw, F), BF16),
        ),
        in_specs=[anywhere] * 5,
        out_specs=(vmem,) * 3,
        scratch_shapes=[
            pltpu.VMEM((3, B, NX, half, quarter), BF16),
            pltpu.VMEM((2, Rw, F), BF16),
            pltpu.VMEM((2, A, B, Rw, 2 * Fs), BF16),
            pltpu.VMEM((2, B * half, 2 * Fs), BF16),
            pltpu.VMEM((2, B, NX, half, quarter), BF16),
            *pair((NX, B, half, v[0]), (NX, B, half, v[1])),
            *pair((B, NX, half, u[0]), (B, NX, half, u[1])),
            *pair((B, half, v[0]), (B, half, v[1])),
            *pair((NX, half, u[0]), (NX, half, u[1])),
            *pair((B, half, v[0]), (B, half, v[1])),
            *pair((NX, half, u[0]), (NX, half, u[1])),
            pltpu.VMEM((A, depth, Fs), BF16),
            pltpu.VMEM((A, depth, Fs), BF16),
            pltpu.VMEM((A, depth, Fs), F32),
            pltpu.VMEM((2, A // 2, depth, Fs), BF16),
            pltpu.VMEM((2, A // 2, depth, Fs), BF16),
            pltpu.VMEM((B, Rw, Fs), BF16),
            dma((3, NX)), dma((4,)),
            dma((B - 1,)), dma((B,)),
            dma((2, A // 4, B, 2)), dma((A, B)),
            dma((A,)), dma((A,)),
            dma((3, B - 1)), dma((3, B)),
            dma((3, B - 1)), dma((3, B)),
            dma((3, B - 1, NX - 1)), dma((3, B, NX)),
            dma((NX,)), dma((NX,)),
            dma((2, A // 2)), dma((2, A // 2)),
            dma((B - 1,)), dma((B,)),
            dma((2, NX - 1)), dma((2, NX)),
            dma((2, B - 1)), dma((2, B)),
            dma((2, B - 1)), dma((2, B)),
            dma((2, NX - 1)), dma((2, NX)),
            dma((2, NX - 1)), dma((2, NX)),
            dma((2, NX)), dma((2, NX)),
        ],
        compiler_params=pltpu.CompilerParams(
            collective_id=0, has_side_effects=True, vmem_limit_bytes=58 * 2**20
        ),
        cost_estimate=pl.CostEstimate(flops=flops, bytes_accessed=2**25, transcendentals=0),
    )(fwd_input, saved_input, out_cotangent, up_weight, down_weight.T)
    grad_part = grad.astype(F32)
    grad_scale = float(rows * n) ** (-0.5)
    return (layer_out, input_grad, up_grad_sum + grad_part * grad_scale)


def solution(mesh):
    placed = (
        P("fs", None),
        P("fs", None),
        P("fs", None),
        P("fs", "tp"),
        P("tp", "fs"),
        P("fs", "tp"),
    )
    return jax.shard_map(
        functools.partial(per_device, mesh.shape["fs"], mesh.shape["tp"]),
        mesh=mesh,
        in_specs=placed,
        out_specs=(P("fs", None), P("fs", None), P("fs", "tp")),
        check_vma=False,
    )
```
